32 devices in a mesh: ep: 4 (over y, x), tp: 8 (over z, core).
Axes of the slice: x: 2, y: 2, z: 4, core: 2. Of those that a mesh axis runs over, the one named last changes fastest.
Arguments:
- tokens: bfloat16 [64, 4096], P('ep'), may hold values from -6 to 6
- attn_gain: float32 [4096], replicated, may hold values from 0.1 to 1.9
- w_query: bfloat16 [4096, 2048], P('ep', 'tp'), may hold values from -0.15625 to 0.15625
- w_key: bfloat16 [4096, 2048], P('ep', 'tp'), may hold values from -0.09375 to 0.09375
- w_value: bfloat16 [4096, 2048], P('ep', 'tp'), may hold values from -0.09375 to 0.09375
- mix_lambda: float32 [16], P('tp'), may hold values from 0.3 to 0.8
- head_gain: float32 [128], replicated, may hold values from 0.1 to 1.9
- w_output: bfloat16 [2048, 4096], P('tp'), may hold values from -0.125 to 0.125
- cache_keys: bfloat16 [64, 1024, 2048], P('ep', None, 'tp'), may hold values from -180 to 180
- cache_value: bfloat16 [64, 1024, 2048], P('ep', None, 'tp'), may hold values from -6 to 6
- lengths: int32 [64], P('ep'), may hold values from 1 to 1024
- moe_gain: float32 [4096], replicated, may hold values from 0.1 to 1.9
- group_ids: int32 [64], P('ep'), may hold values from 0 to 1, as said below
- member_ids: int32 [64, 2], P('ep'), may hold values from 0 to 1, as said below
- group_gate: float32 [64], P('ep'), may hold values from 0.3 to 1
- member_logits: float32 [64, 2], P('ep'), may hold values from -4 to 4
- w_exp_gate: bfloat16 [4, 4096, 2048], P('ep', None, 'tp'), may hold values from -0.09375 to 0.09375
- w_exp_up: bfloat16 [4, 4096, 2048], P('ep', None, 'tp'), may hold values from -0.09375 to 0.09375
- w_exp_down: bfloat16 [4, 2048, 4096], P('ep', 'tp'), may hold values from -0.125 to 0.125
Outputs:
- mixed: bfloat16 [64, 4096], P('ep', 'tp')
- fresh_keys: bfloat16 [64, 2048], P('ep', 'tp')
- fresh_value: bfloat16 [64, 2048], P('ep', 'tp')
The draws below stay inside these ranges and needn't reach their ends.
Inputs may be any that keep to these rules, and one draw needn't show every extreme that they name: `group_ids`: each index of ep holds 16 consecutive tokens, of which every group gets the same number. A token's 2 members differ, and every expert group_ids * 2 + member_ids receives exactly 8 of the token-expert pairs of each index of ep.
All inputs are finite; a program needn't handle non-finite values.
Results may differ from the reference program's by a relative error of at most 0.015.
The reference program's roundings to bfloat16 on the way count: a program that leaves them out, or rounds other values in their place, can miss the bound.
Values may be sent and summed in bfloat16 or wider, within the bound.
A program may use at most 64 MiB of HBM per device.

```python
import jax
import jax.numpy as jnp
from jax import lax

D = 4096
HEADS = 16
DH = 64
FF = 2048
EPG = 2
TOPK = 2
SEQ_DEV = 16
CACHE = 1024
EXPERTS = 4
GROUPS = 2
BATCH = 64
N_EP = 4
N_TP = 8


def routing_tables(key):
    perm_key, start_key, shift_key = jax.random.split(jax.random.fold_in(key, 11), 3)
    perms = jax.vmap(lambda sub: jax.random.permutation(sub, SEQ_DEV))(jax.random.split(perm_key, N_EP))
    starts = jax.random.randint(start_key, (N_EP, GROUPS), 0, EPG)
    shifts = jax.random.randint(shift_key, (N_EP, GROUPS), 1, EPG)
    group = perms % GROUPS
    inside = perms // GROUPS
    start_row = jnp.take_along_axis(starts, group, axis=1)
    shift_row = jnp.take_along_axis(shifts, group, axis=1)
    first = (start_row + inside) % EPG
    second = (start_row + inside + shift_row) % EPG
    members = jnp.stack([first, second], axis=-1)
    return (group.reshape(BATCH).astype(jnp.int32), members.reshape(BATCH, TOPK).astype(jnp.int32))


def draw_group_ids(key, part):
    group, members = routing_tables(key)
    return group


def draw_member_ids(key, part):
    group, members = routing_tables(key)
    return members


def draw_cache_keys(key, part):
    base_key = jax.random.fold_in(jax.random.fold_in(key, 21), 0)
    base = jax.random.truncated_normal(base_key, -6.0, 6.0, (BATCH, CACHE, HEADS * 2 * DH), jnp.float32)
    return base.astype(jnp.bfloat16)


def touch_ends(entries, key, least, top_value):
    place = [jax.random.randint(jax.random.fold_in(key, axis), (), 0, length) for axis, length in enumerate(entries.shape)]
    main_axis = entries.shape.index(max(entries.shape))
    next_to = place[:main_axis] + [(place[main_axis] + 1) % entries.shape[main_axis]] + place[main_axis + 1:]
    return entries.at[tuple(place)].set(least).at[tuple(next_to)].set(top_value)


def block_levels(key, dims, cuts, smallest, largest):
    loudness, own = 1.0, jax.random.fold_in(key, 6)
    for dim, blocks in cuts:
        draws = jnp.exp(jax.random.uniform(jax.random.fold_in(own, dim), (blocks,), jnp.float32, smallest / len(cuts), largest / len(cuts)))
        loudness = loudness * jnp.repeat(draws, dims[dim] // blocks).reshape([-1 if axis == dim else 1 for axis in range(len(dims))])
    return loudness


def gaussian(rng, dims, width, most, shards=(), held_as=jnp.bfloat16):
    level = block_levels(rng, dims, shards, -0.22, 0.18) if shards else 1.0
    values = jax.random.normal(rng, dims, jnp.float32) * width * level
    return jnp.minimum(jnp.maximum(values, -most), most).astype(held_as)


def setup_inputs(seed: int = 0) -> dict:
    key_of = jax.random.split(jax.random.key(seed), 20)
    return {
        "tokens": gaussian(key_of[0], (BATCH, D), 1.0, 6.0, ((0, 4),)),
        "attn_gain": jnp.clip(1.0 + 0.18 * jax.random.normal(key_of[1], (D,), jnp.float32), 0.1, 1.9),
        "w_query": gaussian(key_of[2], (D, HEADS * 2 * DH), (D // 3) ** -0.5, 0.15625, ((0, 4), (1, 8))),
        "w_key": gaussian(key_of[3], (D, HEADS * 2 * DH), D ** -0.5, 0.09375, ((0, 4), (1, 8))),
        "w_value": gaussian(key_of[4], (D, HEADS * 2 * DH), D ** -0.5, 0.09375, ((0, 4), (1, 8))),
        "mix_lambda": jnp.clip(0.3 + 0.5 * jax.random.uniform(key_of[5], (HEADS,), jnp.float32) ** block_levels(key_of[5], (HEADS,), ((0, 8),), -0.2, 0.2), 0.3, 0.8),
        "head_gain": jnp.clip(1.0 + 0.18 * jax.random.normal(key_of[6], (2 * DH,), jnp.float32), 0.1, 1.9),
        "w_output": gaussian(key_of[7], (HEADS * 2 * DH, D), (HEADS * 2 * DH) ** -0.5, 0.125, ((0, 8),)),
        "cache_keys": draw_cache_keys(jax.random.fold_in(key_of[19], 71), 0),
        "cache_value": gaussian(key_of[9], (BATCH, CACHE, HEADS * 2 * DH), 1.0, 6.0, ((0, 4), (2, 8))),
        "lengths": touch_ends(jax.random.randint(key_of[10], (BATCH,), 1, CACHE + 1), jax.random.fold_in(key_of[10], 1), 1, CACHE).astype(jnp.int32),
        "moe_gain": jnp.clip(1.0 + 0.18 * jax.random.normal(key_of[11], (D,), jnp.float32), 0.1, 1.9),
        "group_ids": draw_group_ids(jax.random.fold_in(key_of[19], 71), 0),
        "member_ids": draw_member_ids(jax.random.fold_in(key_of[19], 71), 0),
        "group_gate": jnp.clip(0.3 + 0.7 * jax.random.uniform(key_of[14], (BATCH,), jnp.float32) ** block_levels(key_of[14], (BATCH,), ((0, 4),), -0.2, 0.2), 0.3, 1.0),
        "member_logits": gaussian(key_of[15], (BATCH, TOPK), 1.0, 4.0, ((0, 4),), jnp.float32),
        "w_exp_gate": gaussian(key_of[16], (EXPERTS, D, FF), D ** -0.5, 0.09375, ((0, 4), (2, 8))),
        "w_exp_up": gaussian(key_of[17], (EXPERTS, D, FF), D ** -0.5, 0.09375, ((0, 4), (2, 8))),
        "w_exp_down": gaussian(key_of[18], (EXPERTS, FF, D), FF ** -0.5, 0.125, ((0, 4), (1, 8))),
    }


EPS = 1e-06

def rms_scale(values, gain):
    return values * lax.rsqrt(lax.optimization_barrier(jnp.mean(values * values, axis=-1, keepdims=True)) + EPS) * gain

def reference(tokens, attn_gain, w_query, w_key, w_value, mix_lambda, head_gain, w_output, cache_keys, cache_value, lengths, moe_gain, group_ids, member_ids, group_gate, member_logits, w_exp_gate, w_exp_up, w_exp_down):
    resid_in = tokens.astype(jnp.float32)
    normed = rms_scale(resid_in, attn_gain).astype(jnp.bfloat16)

    def project(weight):
        return jnp.dot(normed, weight, preferred_element_type=jnp.float32).astype(jnp.bfloat16)
    query = project(w_query)
    fresh_keys = project(w_key)
    fresh_val = project(w_value)
    head_index = jnp.arange(HEADS).astype(jnp.float32)
    slopes = 2.0 ** (-8.0 * (head_index + 1.0) / HEADS)
    scale = DH ** (-0.5)
    lam = mix_lambda.astype(jnp.float32)

    def block(args):
        qry, knew, vnew, ckeys, cval, lens = args
        count = qry.shape[0]
        positions = jnp.arange(CACHE)
        dist = (lens[:, None] - positions[None, :]).astype(jnp.float32)
        valid = positions[None, :] < lens[:, None]
        qf = qry.reshape(count, HEADS, 2, DH).astype(jnp.float32)
        keys = ckeys.reshape(count, CACHE, HEADS, 2, DH).astype(jnp.float32)
        fresh = knew.reshape(count, HEADS, 2, DH).astype(jnp.float32)
        old = jnp.einsum('shcd,slhcd->cshl', qf, keys, precision=lax.Precision.HIGHEST) * scale
        old = old - slopes[None, None, :, None] * dist[None, :, None, :]
        old = jnp.where(valid[None, :, None, :], old, -jnp.inf)
        new = jnp.moveaxis(lax.optimization_barrier(jnp.sum(qf * fresh, axis=-1)) * scale, 2, 0)
        full = jnp.concatenate([old, new[..., None]], axis=-1)
        maps = jax.nn.softmax(full, axis=-1)
        weights = (maps[0] - lam[None, :, None] * maps[1]).astype(jnp.bfloat16)
        values = cval.reshape(count, CACHE, HEADS, 2 * DH).astype(jnp.float32)
        wide = weights.astype(jnp.float32)
        head_mix = jnp.einsum('shl,slhe->she', wide[..., :CACHE], values, precision=lax.Precision.HIGHEST)
        head_mix = head_mix + wide[..., CACHE][..., None] * vnew.reshape(count, HEADS, 2 * DH).astype(jnp.float32)
        head_out = rms_scale(head_mix, head_gain).astype(jnp.bfloat16)
        return head_out.reshape(count, HEADS * 2 * DH)

    def split(array):
        return array.reshape((N_EP, SEQ_DEV) + array.shape[1:])
    pieces = (split(query), split(fresh_keys), split(fresh_val), split(cache_keys), split(cache_value), split(lengths))
    head_out = lax.map(block, pieces).reshape(BATCH, HEADS * 2 * DH)
    group = HEADS * 2 * DH // N_TP
    attn_sum = jnp.zeros((BATCH, D), jnp.float32)
    for index in range(N_TP):
        term = jnp.dot(head_out[:, index * group:(index + 1) * group], w_output[index * group:(index + 1) * group], preferred_element_type=jnp.float32).astype(jnp.bfloat16)
        attn_sum = attn_sum + lax.optimization_barrier(term).astype(jnp.float32)
    resid = resid_in + attn_sum
    moe_in = rms_scale(resid, moe_gain).astype(jnp.bfloat16)
    expert_ids = group_ids[:, None] * EPG + member_ids
    route_weight = jax.nn.softmax(member_logits.astype(jnp.float32), axis=-1) * group_gate[:, None]

    def step(total, args):
        gate_w, up_w, down_w, index = args
        gate = jnp.dot(moe_in, gate_w, preferred_element_type=jnp.float32)
        upper = jnp.dot(moe_in, up_w, preferred_element_type=jnp.float32)
        hidden = (jax.nn.silu(gate) * upper).astype(jnp.bfloat16)
        result = jnp.dot(hidden, down_w, preferred_element_type=jnp.float32).astype(jnp.bfloat16)
        share = lax.optimization_barrier(jnp.sum(jnp.where(expert_ids == index, route_weight, 0.0), axis=1))
        return (total + share[:, None] * lax.optimization_barrier(result).astype(jnp.float32), None)
    routed, _ = lax.scan(step, jnp.zeros((BATCH, D), jnp.float32), (w_exp_gate, w_exp_up, w_exp_down, jnp.arange(EXPERTS).astype(jnp.int32)))
    mixed = (resid + routed).astype(jnp.bfloat16)
    return (mixed, fresh_keys, fresh_val)
```

```python
import functools

import jax
import jax.numpy as jnp
from jax import lax
from jax.experimental import pallas as pl
from jax.experimental.pallas import tpu as pltpu
from jax.sharding import PartitionSpec as P

EPG = 2
EPS = 1e-06
MESH = pl.DeviceIdType.MESH
F32 = jnp.float32
BF16 = jnp.bfloat16
GROUP = 4


def iota(shape, dim):
    return lax.broadcasted_iota(jnp.int32, shape, dim)


def layer_kernel(
    n_ep, n_tp, cap,
    tokens, attn_gain, head_gain, moe_gain, lam, lengths, eids, group_gate, logits,
    w_query, w_key, w_value, cache_keys, cache_value, w_output, w_gate, w_up, w_down,
    mixed, fresh_keys, fresh_value,
    wq, wk, wv, kbuf, vbuf, wo, wg, wu, wd,
    nsend, nrecv, psend, precv, query, fkey, fval, head_out,
    tsend, trecv, qsend, qrecv, dsend, drecv, csend, crecv,
    w_sem, c_sem, n_ss, n_rs, p_ss, p_rs, t_ss, t_rs, q_ss, q_rs, d_ss, d_rs, e_ss, e_rs,
):
    ep = lax.axis_index("ep")
    tp = lax.axis_index("tp")
    devices = n_ep * n_tp
    me = ep * n_tp + tp
    seqs, width = tokens.shape
    rows_local = width // n_ep
    qk_cols = w_query.shape[1]
    heads_local = lam.shape[0]
    pair = qk_cols // heads_local
    head_dim = pair // 2
    total_heads = heads_local * n_tp
    positions = cache_keys.shape[1]
    cols = width // n_tp
    slot_rows = dsend.shape[1]
    slots = n_ep * slot_rows

    barrier = pltpu.get_barrier_semaphore()

    def greet(d, carry):
        other = lax.rem(me + d, devices)
        pl.semaphore_signal(
            barrier, inc=1, device_id={"ep": other // n_tp, "tp": lax.rem(other, n_tp)}, device_id_type=MESH
        )
        return carry

    lax.fori_loop(1, devices, greet, 0)

    weight_pairs = [(w_query, wq), (w_key, wk), (w_value, wv), (w_output, wo), (w_gate, wg), (w_up, wu), (w_down, wd)]

    def weight_copy(i):
        return pltpu.make_async_copy(weight_pairs[i][0], weight_pairs[i][1], w_sem.at[i])

    def cache_copy(g, kind):
        src, dst = ((cache_keys, kbuf), (cache_value, vbuf))[kind]
        rows = pl.ds(g * GROUP, GROUP)
        return pltpu.make_async_copy(src.at[rows], dst.at[rows], c_sem.at[kind, g])

    for i in range(3):
        weight_copy(i).start()
    for g in range(seqs // GROUP):
        cache_copy(g, 0).start()
        cache_copy(g, 1).start()
    for i in range(3, 7):
        weight_copy(i).start()

    resid_in = tokens[...].astype(F32)
    inv = lax.rsqrt(jnp.mean(resid_in * resid_in, axis=-1, keepdims=True) + EPS)
    normed = (resid_in * inv * attn_gain[...]).astype(BF16)
    for e in range(n_ep):
        nsend[e] = normed[:, e * rows_local : (e + 1) * rows_local]
    nrecv[ep] = nsend[ep]

    pl.semaphore_wait(barrier, devices - 1)

    def over_ep(send, recv, ss, rs, d):
        other = lax.rem(ep + d, n_ep)
        return pltpu.make_async_remote_copy(
            src_ref=send.at[other], dst_ref=recv.at[ep], send_sem=ss.at[d], recv_sem=rs.at[d],
            device_id={"ep": other, "tp": tp}, device_id_type=MESH,
        )

    for d in range(1, n_ep):
        over_ep(nsend, nrecv, n_ss, n_rs, d).start()
    for i in range(3):
        weight_copy(i).wait()
    for d in range(1, n_ep):
        over_ep(nsend, nrecv, n_ss, n_rs, d).wait_recv()
    rows_all = nrecv[...].reshape(n_ep * seqs, rows_local)
    for i, w in enumerate((wq, wk, wv)):
        part = jnp.dot(rows_all, w[...], preferred_element_type=F32)
        psend[:, :, i * qk_cols : (i + 1) * qk_cols] = part.reshape(n_ep, seqs, qk_cols)
    for d in range(1, n_ep):
        over_ep(psend, precv, p_ss, p_rs, d).start()
    precv[ep] = psend[ep]

    slot = iota((seqs, slots), 1)
    expert_of = slot // slot_rows
    rank_of = (slot % slot_rows).astype(F32)
    hits = [eids[:, k : k + 1] == expert_of for k in range(2)]
    used = (hits[0] | hits[1]).astype(BF16)
    lower = (iota((seqs, seqs), 1) < iota((seqs, seqs), 0)).astype(BF16)
    ranks = jnp.dot(lower, used, preferred_element_type=F32)
    in_slot = ranks == rank_of
    chosen = [(hits[k] & in_slot).astype(F32) for k in range(2)]
    picker = (chosen[0] + chosen[1]).T.astype(BF16)
    lg = logits[...]
    ex = jnp.exp(lg - jnp.max(lg, axis=-1, keepdims=True))
    route = ex / jnp.sum(ex, axis=-1, keepdims=True) * group_gate[...]

    for d in range(1, n_ep):
        over_ep(psend, precv, p_ss, p_rs, d).wait_recv()
    total = precv[0]
    for e in range(1, n_ep):
        total = total + precv[e]
    projected = total.astype(BF16)
    fresh_keys[...] = projected[:, qk_cols : 2 * qk_cols]
    fresh_value[...] = projected[:, 2 * qk_cols :]
    projected = projected.astype(F32)
    query[...] = projected[:, :qk_cols]
    fkey[...] = projected[:, qk_cols : 2 * qk_cols]
    fval[...] = projected[:, 2 * qk_cols :]

    scale = head_dim ** (-0.5)
    row16 = iota((16, qk_cols), 0)
    col16 = iota((16, qk_cols), 1)
    map_mask = ((col16 // pair == row16 % 8) & ((col16 // head_dim) % 2 == row16 // 8)).astype(F32)
    head_mask = (iota((8, qk_cols), 1) // pair == iota((8, qk_cols), 0)).astype(F32)
    head_row = (tp * heads_local + iota((16, 1), 0) % 8).astype(F32)
    slopes = jnp.exp2(-8.0 * (head_row + 1.0) / total_heads)
    lam_col = jnp.zeros((8, 1), F32)
    for h in range(heads_local):
        lam_col = jnp.where(iota((8, 1), 0) == h, lam[h], lam_col)
    gain_row = jnp.concatenate([head_gain[...]] * heads_local, axis=1)
    spots = iota((1, positions), 1)

    def attend(g, carry):
        cache_copy(g, 0).wait()
        cache_copy(g, 1).wait()
        olds, news = [], []
        for i in range(GROUP):
            s = g * GROUP + i
            q16 = query[pl.ds(s, 1), :] * map_mask
            old = lax.dot_general(
                q16.astype(BF16), kbuf[s], (((1,), (1,)), ((), ())), preferred_element_type=F32
            )
            n = lengths[s]
            old = old * scale - slopes * (n - spots).astype(F32)
            olds.append(jnp.where(spots < n, old, -jnp.inf))
            news.append(jnp.sum(q16 * fkey[pl.ds(s, 1), :], axis=-1, keepdims=True) * scale)
        for i in range(GROUP):
            s = g * GROUP + i
            top = jnp.maximum(jnp.max(olds[i], axis=-1, keepdims=True), news[i])
            old = jnp.exp(olds[i] - top)
            new = jnp.exp(news[i] - top)
            recip = 1.0 / (jnp.sum(old, axis=-1, keepdims=True) + new)
            old = old * recip
            new = new * recip
            weights = (old[:8] - lam_col * old[8:]).astype(BF16)
            fresh = (new[:8] - lam_col * new[8:]).astype(BF16).astype(F32)
            mix = jnp.dot(weights, vbuf[s], preferred_element_type=F32)
            mix = (mix + fresh * fval[pl.ds(s, 1), :]) * head_mask
            mean = jnp.sum(mix * mix, axis=-1, keepdims=True) / pair
            mix = mix * lax.rsqrt(mean + EPS) * gain_row
            head_out[pl.ds(s, 1), :] = jnp.sum(mix, axis=0, keepdims=True)
        return carry

    lax.fori_loop(0, seqs // GROUP, attend, 0)

    weight_copy(3).wait()
    heads = head_out[...].astype(BF16)
    for t in range(n_tp):
        tsend[t] = jnp.dot(
            heads, wo[:, t * cols : (t + 1) * cols], preferred_element_type=F32
        ).astype(BF16)

    def over_tp(send, recv, ss, rs, d, same=False):
        other = lax.rem(tp + d, n_tp)
        return pltpu.make_async_remote_copy(
            src_ref=send if same else send.at[other], dst_ref=recv.at[tp], send_sem=ss.at[d], recv_sem=rs.at[d],
            device_id={"ep": ep, "tp": other}, device_id_type=MESH,
        )

    for d in range(1, n_tp):
        over_tp(tsend, trecv, t_ss, t_rs, d).start()
    trecv[tp] = tsend[tp]
    for d in range(1, n_tp):
        over_tp(tsend, trecv, t_ss, t_rs, d).wait_recv()
    attn = trecv[0].astype(F32)
    for t in range(1, n_tp):
        attn = attn + trecv[t].astype(F32)
    my_cols = pl.ds(pl.multiple_of(tp * cols, cols), cols)
    resid = tokens[:, my_cols].astype(F32) + attn
    squares = jnp.sum(resid * resid, axis=-1, keepdims=True)
    qsend[...] = jnp.broadcast_to(squares, qsend.shape)
    for d in range(1, n_tp):
        over_tp(qsend, qrecv, q_ss, q_rs, d, True).start()
    qrecv[tp] = qsend[...]
    for d in range(1, n_tp):
        over_tp(qsend, qrecv, q_ss, q_rs, d, True).wait_recv()
    squares = qrecv[0]
    for t in range(1, n_tp):
        squares = squares + qrecv[t]
    inv = lax.rsqrt(squares[:, :1] / width + EPS)
    moe_in = (resid * inv * moe_gain[:, my_cols]).astype(BF16)
    dispatch = jnp.dot(picker, moe_in, preferred_element_type=F32)
    for e in range(n_ep):
        dsend[e] = dispatch[e * slot_rows : (e + 1) * slot_rows].astype(BF16)

    def spread(d):
        other = lax.rem(me + d, devices)
        other_ep, other_tp = other // n_tp, lax.rem(other, n_tp)
        return pltpu.make_async_remote_copy(
            src_ref=dsend.at[other_ep], dst_ref=drecv.at[tp, ep], send_sem=d_ss.at[d], recv_sem=d_rs.at[d],
            device_id={"ep": other_ep, "tp": other_tp}, device_id_type=MESH,
        )

    def gather(d):
        other = lax.rem(me + d, devices)
        other_ep, other_tp = other // n_tp, lax.rem(other, n_tp)
        return pltpu.make_async_remote_copy(
            src_ref=csend.at[other_tp, other_ep], dst_ref=crecv.at[tp, ep], send_sem=e_ss.at[d], recv_sem=e_rs.at[d],
            device_id={"ep": other_ep, "tp": other_tp}, device_id_type=MESH,
        )

    def each(action):
        def step(d, carry):
            action(d)
            return carry

        lax.fori_loop(1, devices, step, 0)

    each(lambda d: spread(d).start())
    drecv[tp, ep] = dsend[ep]
    weight_copy(4).wait()
    weight_copy(5).wait()
    each(lambda d: spread(d).wait_recv())
    gate = jnp.zeros((slots, w_gate.shape[2]), F32)
    upper = gate
    for t in range(n_tp):
        rows = drecv[t].astype(F32).reshape(slots, cols).astype(BF16)
        gate = gate + jnp.dot(rows, wg[0, t * cols : (t + 1) * cols], preferred_element_type=F32)
        upper = upper + jnp.dot(rows, wu[0, t * cols : (t + 1) * cols], preferred_element_type=F32)
    hidden = (gate / (1.0 + jnp.exp(-gate)) * upper).astype(BF16)
    weight_copy(6).wait()
    for t in range(n_tp):
        down = jnp.dot(hidden, wd[0, :, t * cols : (t + 1) * cols], preferred_element_type=F32)
        csend[t] = down.reshape(n_ep, slot_rows, cols).astype(BF16)
    each(lambda d: gather(d).start())
    crecv[tp, ep] = csend[tp, ep]
    each(lambda d: gather(d).wait_recv())
    out = crecv[0].astype(F32)
    for t in range(1, n_tp):
        out = out + crecv[t].astype(F32)
    out = out.reshape(slots, cols).astype(BF16)
    routed = jnp.zeros((seqs, cols), F32)
    for k in range(2):
        picked = jnp.dot(chosen[k].astype(BF16), out, preferred_element_type=F32)
        routed = routed + route[:, k : k + 1] * picked
    mixed[...] = (resid + routed).astype(BF16)

    for d in range(1, n_ep):
        over_ep(nsend, nrecv, n_ss, n_rs, d).wait_send()
        over_ep(psend, precv, p_ss, p_rs, d).wait_send()
    for d in range(1, n_tp):
        over_tp(tsend, trecv, t_ss, t_rs, d).wait_send()
        over_tp(qsend, qrecv, q_ss, q_rs, d, True).wait_send()
    each(lambda d: spread(d).wait_send())
    each(lambda d: gather(d).wait_send())


def on_device(
    tokens, attn_gain, w_query, w_key, w_value, mix_lambda, head_gain, w_output, cache_keys, cache_value,
    lengths, moe_gain, group_ids, member_ids, group_gate, member_logits, w_exp_gate, w_exp_up, w_exp_down,
):
    n_ep, n_tp = lax.axis_size("ep"), lax.axis_size("tp")
    seqs, width = tokens.shape
    qk_cols = w_query.shape[1]
    experts_all = w_exp_gate.shape[0] * n_ep
    cap = seqs * member_ids.shape[1] // experts_all
    slot_rows = -(-cap // 8) * 8
    cols = width // n_tp
    devices = n_ep * n_tp
    eids = group_ids[:, None] * EPG + member_ids
    vmem = pl.BlockSpec(memory_space=pltpu.VMEM)
    smem = pl.BlockSpec(memory_space=pltpu.SMEM)
    hbm = pl.BlockSpec(memory_space=pl.ANY)
    dma = pltpu.SemaphoreType.DMA
    like = lambda a: pltpu.VMEM(a.shape, a.dtype)
    scratch = [
        like(w_query), like(w_key), like(w_value), like(cache_keys), like(cache_value),
        like(w_output), like(w_exp_gate), like(w_exp_up), like(w_exp_down),
        pltpu.VMEM((n_ep, seqs, width // n_ep), BF16),
        pltpu.VMEM((n_ep, seqs, width // n_ep), BF16),
        pltpu.VMEM((n_ep, seqs, 3 * qk_cols), F32),
        pltpu.VMEM((n_ep, seqs, 3 * qk_cols), F32),
        pltpu.VMEM((seqs, qk_cols), F32),
        pltpu.VMEM((seqs, qk_cols), F32),
        pltpu.VMEM((seqs, qk_cols), F32),
        pltpu.VMEM((seqs, qk_cols), F32),
        pltpu.VMEM((n_tp, seqs, cols), BF16),
        pltpu.VMEM((n_tp, seqs, cols), BF16),
        pltpu.VMEM((seqs, 128), F32),
        pltpu.VMEM((n_tp, seqs, 128), F32),
        pltpu.VMEM((n_ep, slot_rows, cols), BF16),
        pltpu.VMEM((n_tp, n_ep, slot_rows, cols), BF16),
        pltpu.VMEM((n_tp, n_ep, slot_rows, cols), BF16),
        pltpu.VMEM((n_tp, n_ep, slot_rows, cols), BF16),
        dma((7,)), dma((2, seqs // GROUP)),
        dma((n_ep,)), dma((n_ep,)), dma((n_ep,)), dma((n_ep,)),
        dma((n_tp,)), dma((n_tp,)), dma((n_tp,)), dma((n_tp,)),
        dma((devices,)), dma((devices,)), dma((devices,)), dma((devices,)),
    ]
    return pl.pallas_call(
        functools.partial(layer_kernel, n_ep, n_tp, cap),
        out_shape=(
            jax.ShapeDtypeStruct((seqs, cols), BF16),
            jax.ShapeDtypeStruct((seqs, qk_cols), BF16),
            jax.ShapeDtypeStruct((seqs, qk_cols), BF16),
        ),
        in_specs=[vmem] * 4 + [smem] * 2 + [vmem] * 3 + [hbm] * 9,
        out_specs=(vmem, vmem, vmem),
        scratch_shapes=scratch,
        compiler_params=pltpu.CompilerParams(
            collective_id=0, has_side_effects=True, vmem_limit_bytes=60 * 1024 * 1024
        ),
        name="decode_layer",
    )(
        tokens, attn_gain[None, :], head_gain[None, :], moe_gain[None, :], mix_lambda, lengths,
        eids, group_gate[:, None], member_logits,
        w_query, w_key, w_value, cache_keys, cache_value, w_output, w_exp_gate, w_exp_up, w_exp_down,
    )


def solution(mesh):
    return jax.shard_map(
        on_device,
        mesh=mesh,
        in_specs=(
            P("ep", None),
            P(),
            P("ep", "tp"),
            P("ep", "tp"),
            P("ep", "tp"),
            P("tp"),
            P(),
            P("tp", None),
            P("ep", None, "tp"),
            P("ep", None, "tp"),
            P("ep"),
            P(),
            P("ep"),
            P("ep", None),
            P("ep"),
            P("ep", None),
            P("ep", None, "tp"),
            P("ep", None, "tp"),
            P("ep", "tp", None),
        ),
        out_specs=(P("ep", "tp"), P("ep", "tp"), P("ep", "tp")),
        check_vma=False,
    )
```
